32 devices in a mesh: fs: 8 (over z, y), tp: 4 (over x, core).
Axes of the slice: x: 2, y: 2, z: 4, core: 2. Of those that a mesh axis runs over, the one named last changes fastest.
Arguments:
- resid: bfloat16 [8192, 2048], P(('fs', 'tp')), may hold values from -6 to 6
- mix_gain: float32 [2048], replicated, may hold values from 0.1 to 1.9
- w_query: bfloat16 [2048, 1024], P('fs', 'tp'), may hold values from -0.125 to 0.125
- w_key: bfloat16 [2048, 1024], P('fs', 'tp'), may hold values from -0.125 to 0.125
- w_value: bfloat16 [2048, 2048], P('fs', 'tp'), may hold values from -0.125 to 0.125
- w_gate: bfloat16 [2048, 2048], P('fs', 'tp'), may hold values from -0.125 to 0.125
- w_output: bfloat16 [2048, 2048], P('tp', 'fs'), may hold values from -0.125 to 0.125
- decay_rate: float32 [8], P('tp'), may hold values from 0.0008 to 0.034, as said below
- mlp_gain: float32 [2048], replicated, may hold values from 0.1 to 1.9
- w_up: bfloat16 [2048, 8192], P('fs', 'tp'), may hold values from -0.125 to 0.125
- w_down: bfloat16 [8192, 2048], P('tp', 'fs'), may hold values from -0.0625 to 0.0625
Outputs:
- layer_out: bfloat16 [8192, 2048], P(('fs', 'tp'))
The draws below stay inside these ranges and needn't reach their ends.
Inputs may be any that keep to these rules, and one draw needn't show every extreme that they name: `decay_rate`: decay rates per position, one for each head.
All inputs are finite; a program needn't handle non-finite values.
Results may differ from the reference program's by a relative error of at most 0.038.
Values may be sent and summed in bfloat16 or wider, within the bound.
A program may use at most 64 MiB of HBM per device.

```python
import jax
import jax.numpy as jnp
from jax import lax

D = 2048
HEADS = 8
DK = 128
DV = 256
FF = 8192
BLOCK = 128
LENGTH = 512
TOKENS = 8192
N_TP = 4


def draw_decay_rate(key, part):
    order_key, quick_key, slow_key = jax.random.split(key, 3)
    ranking = jax.random.permutation(order_key, HEADS)
    quick_rate = jnp.exp(jax.random.uniform(quick_key, (HEADS,), jnp.float32, jnp.log(1.0 / 50.0), jnp.log(1.0 / 30.0)))
    slow_rate = jax.random.uniform(slow_key, (HEADS,), jnp.float32, 0.2, 1.0) * (2.3 / LENGTH)
    return jnp.where(ranking < HEADS // 2, quick_rate, slow_rate)


def levels(rng, shape, cuts, low, largest):
    def one(position, shards_of):
        draws = jax.random.uniform(jax.random.fold_in(jax.random.fold_in(rng, 6), position), (shards_of,), jnp.float32, low / len(cuts), largest / len(cuts))
        return jnp.repeat(jnp.exp(draws), shape[position] // shards_of).reshape((-1,) + (1,) * (len(shape) - position - 1))

    level = one(*cuts[0])
    for cut in cuts[1:]:
        level = level * one(*cut)
    return level


def scatter_about(own_key, shape, scale, limit, pieces=(), held_as=jnp.bfloat16):
    drawn = jax.random.normal(own_key, shape, jnp.float32) * scale
    if len(pieces) > 0:
        drawn = levels(own_key, shape, pieces, -0.22, 0.18) * drawn
    return jnp.clip(drawn, min=-limit, max=limit).astype(held_as)


def setup_inputs(seed: int = 0) -> dict:
    key_list = jax.random.split(jax.random.key(seed), 12)
    resid = scatter_about(key_list[0], (TOKENS, D), 1.0, 6.0, ((0, 32),))
    mix_gain = jnp.clip(1.0 + 0.18 * jax.random.normal(key_list[1], (D,), jnp.float32), 0.1, 1.9)
    w_query = scatter_about(key_list[2], (D, HEADS * DK), D ** -0.5, 0.125, ((0, 8), (1, 4)))
    w_key = scatter_about(key_list[3], (D, HEADS * DK), D ** -0.5, 0.125, ((0, 8), (1, 4)))
    w_value = scatter_about(key_list[4], (D, HEADS * DV), D ** -0.5, 0.125, ((0, 8), (1, 4)))
    w_gate = scatter_about(key_list[5], (D, HEADS * DV), D ** -0.5, 0.125, ((0, 8), (1, 4)))
    w_output = scatter_about(key_list[6], (HEADS * DV, D), (HEADS * DV) ** -0.5, 0.125, ((0, 4), (1, 8)))
    decay_rate = draw_decay_rate(jax.random.fold_in(key_list[11], 71), 0)
    mlp_gain = jnp.clip(1.0 + 0.18 * jax.random.normal(key_list[8], (D,), jnp.float32), 0.1, 1.9)
    w_up = scatter_about(key_list[9], (D, FF), D ** -0.5, 0.125, ((0, 8), (1, 4)))
    w_down = scatter_about(key_list[10], (FF, D), FF ** -0.5, 0.0625, ((0, 4), (1, 8)))
    return dict(resid=resid, mix_gain=mix_gain, w_query=w_query, w_key=w_key, w_value=w_value, w_gate=w_gate, w_output=w_output, decay_rate=decay_rate, mlp_gain=mlp_gain, w_up=w_up, w_down=w_down)


epsilon = 1e-06

def rms_scale(source, gains):
    widened = source.astype(jnp.float32)
    scaled = widened * lax.rsqrt(lax.optimization_barrier(jnp.mean(widened * widened, axis=-1, keepdims=True)) + epsilon)
    return (scaled * gains).astype(jnp.bfloat16)

def retention(queries, key_rows, values, rates):
    seq_count, length, head_count, key_width = queries.shape
    value_width = values.shape[-1]
    block_count = length // BLOCK
    queries = queries.reshape(seq_count, block_count, BLOCK, head_count, key_width)
    key_rows = key_rows.reshape(seq_count, block_count, BLOCK, head_count, key_width) * key_width ** (-0.5)
    values = values.reshape(seq_count, block_count, BLOCK, head_count, value_width)
    places = jnp.arange(BLOCK, dtype=jnp.float32)
    offset = places[:, None] - places[None, :]
    causal = offset >= 0
    inner_decay = jnp.where(causal[None], jnp.exp(-rates[:, None, None] * jnp.where(causal, offset, 0.0)[None]), 0.0)
    scores = jnp.einsum('bnihd,bnjhd->bnhij', queries, key_rows) * inner_decay[None, None]
    within = jnp.einsum('bnhij,bnjhe->bnihe', scores, values)
    key_decayed = key_rows * jnp.exp(-rates[None, :] * (BLOCK - 1.0 - places)[:, None])[None, None, :, :, None]
    updates = jnp.einsum('bnjhd,bnjhe->nbhde', key_decayed, values)
    carry_decay = jnp.exp(-rates * BLOCK)[None, :, None, None]

    def advance(memory, update):
        return (carry_decay * memory + update, memory)
    _, before = lax.scan(advance, jnp.zeros((seq_count, head_count, key_width, value_width), jnp.float32), updates)
    query_decayed = queries * jnp.exp(-rates[None, :] * (places + 1.0)[:, None])[None, None, :, :, None]
    carried = jnp.einsum('bnihd,nbhde->bnihe', query_decayed, before)
    mixed = (within + carried).reshape(seq_count, length, head_count, value_width)
    centre = lax.optimization_barrier(jnp.mean(mixed, axis=-1, keepdims=True))
    spread = lax.optimization_barrier(jnp.mean(jnp.square(mixed - centre), axis=-1, keepdims=True))
    return (mixed - centre) * lax.rsqrt(spread + epsilon)

def heads_view(source, width):
    return source.astype(jnp.float32).reshape(-1, LENGTH, source.shape[1] // width, width)

def grouped_sum(left, right):
    group = left.shape[1] // N_TP
    result = jnp.zeros((left.shape[0], right.shape[1]), jnp.float32)
    for member in range(N_TP):
        partial_sum = jnp.dot(left[:, member * group:(member + 1) * group], right[member * group:(member + 1) * group], preferred_element_type=jnp.float32)
        result = result + lax.optimization_barrier(partial_sum.astype(jnp.bfloat16)).astype(jnp.float32)
    return result

def reference(resid, mix_gain, w_query, w_key, w_value, w_gate, w_output, decay_rate, mlp_gain, w_up, w_down):
    tokens = resid.shape[0]
    normed = rms_scale(resid, mix_gain)

    def project(weight):
        return jnp.dot(normed, weight, preferred_element_type=jnp.float32).astype(jnp.bfloat16)
    queries = project(w_query)
    key_rows = project(w_key)
    values = project(w_value)
    gate_rows = project(w_gate)
    grouped = retention(heads_view(queries, DK), heads_view(key_rows, DK), heads_view(values, DV), decay_rate)
    gated = (jax.nn.silu(gate_rows.astype(jnp.float32)) * grouped.reshape(tokens, -1)).astype(jnp.bfloat16)
    mix_sum = grouped_sum(gated, w_output)
    after_mix = (resid.astype(jnp.float32) + mix_sum).astype(jnp.bfloat16)
    normed_mlp = rms_scale(after_mix, mlp_gain)
    lifted = jnp.dot(normed_mlp, w_up, preferred_element_type=jnp.float32)
    hidden = jnp.square(jax.nn.relu(lifted)).astype(jnp.bfloat16)
    mlp_sum = grouped_sum(hidden, w_down)
    return (after_mix.astype(jnp.float32) + mlp_sum).astype(jnp.bfloat16)
```

```python
import functools

import jax
import jax.numpy as jnp
from jax import lax
from jax.experimental import pallas as pl
from jax.experimental.pallas import tpu as pltpu
from jax.sharding import PartitionSpec as P

DK = 128
DV = 256
LENGTH = 512
MESH = pl.DeviceIdType.MESH
EPS = 1e-06
F32 = jnp.float32
BF16 = jnp.bfloat16


def tile_of(width):
    return 256 if width % 256 == 0 else 128


def kernel(fs, tp, resid_ref, mix_gain_ref, mlp_gain_ref, rate_ref, wq_ref, wo_ref, wu_ref, wd_ref,
           out_ref, wq, wo, wu, wd, xn, xn2, proj, gated, hidden, part1, recv1, part2, recv2,
           after, ring_send, ring_recv, own_sem, ag_send, ag_recv, rs1_send, rs1_recv,
           rs2_send, rs2_recv):
    half = fs // 2
    rows = resid_ref.shape[0]
    heads = rate_ref.shape[0]
    tokens = rows * tp
    me_f = lax.axis_index("fs")
    me_t = lax.axis_index("tp")

    def place(i):
        col = i % 2
        line = i // 2
        return line * (1 - col) + (fs - 1 - line) * col

    def index(p):
        col = p // half
        return 2 * (p * (1 - col) + (fs - 1 - p) * col) + col

    my_place = place(me_f)
    target = (index((my_place + 1) % fs), index((my_place + fs - 1) % fs))

    def owner(way, dist):
        if way == 0:
            return index((my_place + fs - dist) % fs)
        return index((my_place + dist) % fs)

    def peer(d):
        return (me_t + d) % tp

    barrier = pltpu.get_barrier_semaphore()
    for way in range(2):
        pl.semaphore_signal(barrier, inc=1, device_id=(target[way], me_t), device_id_type=MESH)
    for d in range(1, tp):
        pl.semaphore_signal(barrier, inc=1, device_id=(me_f, peer(d)), device_id_type=MESH)
    pl.semaphore_wait(barrier, 2 + tp - 1)

    groups = ((wq_ref, wq, False), (wo_ref, wo, True), (wu_ref, wu, False), (wd_ref, wd, True))

    def slot(w, who, h):
        source, whole, slotted = groups[w]
        deep = source.shape[0]
        hr = deep // 2
        if slotted:
            return whole.at[who, pl.ds(h * hr, hr), :]
        return whole.at[pl.ds(pl.multiple_of(who * deep + h * hr, hr), hr), :]

    rounds = []
    for w in range(4):
        for dist in range(1, half):
            rounds += [(w, dist, 0), (w, dist, 1)]
        rounds.append((w, half, 0))
    per = fs - 1
    started = []

    def half_of(way, turn):
        return turn if way == 0 else 1 - turn

    def send(k):
        w, dist, turn = rounds[k]
        for way in range(2):
            h = half_of(way, turn)
            who = owner(way, dist - 1)
            source = groups[w][0]
            hr = source.shape[0] // 2
            src = source.at[pl.ds(h * hr, hr), :] if dist == 1 else slot(w, who, h)
            copy = pltpu.make_async_remote_copy(
                src_ref=src, dst_ref=slot(w, who, h), send_sem=ring_send.at[way, k],
                recv_sem=ring_recv.at[way, k], device_id=(target[way], me_t), device_id_type=MESH)
            copy.start()
            started.append(copy)

    def arrive(k):
        w, dist, turn = rounds[k]
        for way in range(2):
            h = half_of(way, turn)
            here = slot(w, owner(way, dist), h)
            pltpu.make_async_remote_copy(
                src_ref=here, dst_ref=here, send_sem=ring_send.at[way, k],
                recv_sem=ring_recv.at[way, k], device_id=(target[way], me_t),
                device_id_type=MESH).wait_recv()
        if dist + 1 < half or (dist + 1 == half and turn == 0):
            send(k + 2)

    own_at = {}
    own_at.setdefault(per - 3, []).append(per)
    own_at.setdefault(per - 2, []).append(per + 1)
    own_at.setdefault(per - 1, []).append(2 * per)
    own_at.setdefault(per + 3, []).append(2 * per + 1)
    own_at.setdefault(3 * per - 3, []).append(3 * per)
    own_at.setdefault(3 * per - 2, []).append(3 * per + 1)

    send(0)
    send(1)
    own = []
    for w in range(4):
        source, whole, slotted = groups[w]
        deep = source.shape[0]
        dst = whole.at[me_f] if slotted else whole.at[pl.ds(pl.multiple_of(me_f * deep, deep), deep), :]
        copy = pltpu.make_async_copy(source, dst, own_sem.at[w])
        copy.start()
        own.append(copy)

    my_rows = pl.ds(pl.multiple_of(me_t * rows, rows), rows)

    def norm(source, gain_ref):
        wide = source.astype(F32)
        mean = jnp.mean(wide * wide, axis=-1, keepdims=True)
        return (wide * lax.rsqrt(mean + EPS) * gain_ref[...]).astype(BF16)

    def ag_copy(which, buf, d, receiving):
        block = peer(tp - d) if receiving else me_t
        place_ = buf.at[pl.ds(pl.multiple_of(block * rows, rows), rows), :]
        return pltpu.make_async_remote_copy(
            src_ref=place_, dst_ref=place_, send_sem=ag_send.at[which, d - 1],
            recv_sem=ag_recv.at[which, d - 1], device_id=(me_f, peer(d)), device_id_type=MESH)

    def ag_start(which, buf):
        for d in range(1, tp):
            copy = ag_copy(which, buf, d, False)
            copy.start()
            started.append(copy)

    def ag_wait(which, buf):
        for d in range(1, tp):
            ag_copy(which, buf, d, True).wait_recv()

    step = 64

    def norm_into(buf, source_ref, gain_ref):
        @pl.loop(0, rows // step)
        def _(i):
            at = pl.multiple_of(i * step, step)
            buf[pl.ds(pl.multiple_of(me_t * rows + at, step), step), :] = norm(
                source_ref[pl.ds(at, step), :], gain_ref)

    def project():
        width = proj.shape[1]
        t = tile_of(width)

        @pl.loop(0, width // t)
        def _(j):
            cols = pl.ds(pl.multiple_of(j * t, t), t)
            proj[:, cols] = jnp.dot(xn[...], wq[:, cols], preferred_element_type=F32).astype(BF16)

    def retain():
        kq = heads * DK
        vq = heads * DV
        count = tokens // LENGTH
        for head in range(heads):
            rate = rate_ref[head:head + 1, 0:1]

            @pl.loop(0, count)
            def _(n):
                base = pl.multiple_of(n * LENGTH, LENGTH)
                rs = pl.ds(base, LENGTH)
                q = proj[rs, head * DK:(head + 1) * DK]
                k = proj[rs, kq + head * DK:kq + (head + 1) * DK]
                v = proj[rs, 2 * kq + head * DV:2 * kq + (head + 1) * DV]
                g = proj[rs, 2 * kq + vq + head * DV:2 * kq + vq + (head + 1) * DV].astype(F32)
                scores = lax.dot_general(q, k, (((1,), (1,)), ((), ())), preferred_element_type=F32)
                t_at = lax.broadcasted_iota(jnp.int32, (LENGTH, LENGTH), 0)
                s_at = lax.broadcasted_iota(jnp.int32, (LENGTH, LENGTH), 1)
                gap = t_at - s_at
                decay = jnp.exp(-rate * jnp.maximum(gap, 0).astype(F32)) * (DK ** -0.5)
                scores = jnp.where(gap >= 0, scores * decay, 0.0).astype(BF16)
                mixed = jnp.dot(scores, v, preferred_element_type=F32)
                mean = jnp.mean(mixed, axis=-1, keepdims=True)
                off = mixed - mean
                var = jnp.mean(off * off, axis=-1, keepdims=True)
                grouped = off * lax.rsqrt(var + EPS)
                gated[rs, head * DV:(head + 1) * DV] = (g / (1.0 + jnp.exp(-g)) * grouped).astype(BF16)

    def block_of(ref, d, who):
        return ref.at[who, pl.ds(pl.multiple_of(peer(d) * rows, rows), rows), :]

    def reduce_send(part, recv, s_sem, r_sem, who, order):
        for d in range(1, tp):
            copy = pltpu.make_async_remote_copy(
                src_ref=block_of(part, d, who), dst_ref=recv.at[d - 1, who],
                send_sem=s_sem.at[d - 1, order], recv_sem=r_sem.at[d - 1, order],
                device_id=(me_f, peer(d)), device_id_type=MESH)
            copy.start()
            started.append(copy)

    def reduce_wait(recv, s_sem, r_sem, who, order):
        for d in range(1, tp):
            here = recv.at[d - 1, who]
            pltpu.make_async_remote_copy(
                src_ref=here, dst_ref=here, send_sem=s_sem.at[d - 1, order],
                recv_sem=r_sem.at[d - 1, order], device_id=(me_f, peer(d)),
                device_id_type=MESH).wait_recv()

    def total_into(dst_ref, base_ref, part, recv, who):
        width = part.shape[2]
        cols = pl.ds(pl.multiple_of(who * width, width), width)
        total = part[who, my_rows, :].astype(F32)
        for d in range(1, tp):
            total = total + recv[d - 1, who].astype(F32)
        dst_ref[:, cols] = (base_ref[:, cols].astype(F32) + total).astype(BF16)

    def lift():
        width = hidden.shape[1]
        t = tile_of(width)

        @pl.loop(0, width // t)
        def _(j):
            cols = pl.ds(pl.multiple_of(j * t, t), t)
            up = jnp.maximum(jnp.dot(xn2[...], wu[:, cols], preferred_element_type=F32), 0.0)
            hidden[:, cols] = (up * up).astype(BF16)

    def lower(who, order):
        part2[who] = jnp.dot(hidden[...], wd[who], preferred_element_type=F32).astype(BF16)
        reduce_send(part2, recv2, rs2_send, rs2_recv, who, order)

    norm_into(xn, resid_ref, mix_gain_ref)
    ag_start(0, xn)

    def stage(k):
        if k == per - 1:
            own[0].wait()
            ag_wait(0, xn)
            project()
        elif k == per + 1:
            retain()
        elif k == 2 * per - 1:
            own[1].wait()

            @pl.loop(0, fs)
            def _(j):
                part1[j] = jnp.dot(gated[...], wo[j], preferred_element_type=F32).astype(BF16)
            for j in range(fs):
                reduce_send(part1, recv1, rs1_send, rs1_recv, j, j)
        elif k == 3 * per - 3:
            for j in range(fs):
                reduce_wait(recv1, rs1_send, rs1_recv, j, j)

            @pl.loop(0, fs)
            def _(j):
                total_into(after, resid_ref, part1, recv1, j)
            norm_into(xn2, after, mlp_gain_ref)
            ag_start(1, xn2)
        elif k == 3 * per + 2:
            own[2].wait()
            ag_wait(1, xn2)
            lift()
            own[3].wait()
            lower(me_f, 0)
            for dist in range(1, 2):
                for way in range(2):
                    lower(owner(way, dist), 2 * dist - 1 + way)
        elif k > 3 * per + 2:
            _, dist, turn = rounds[k]
            if turn == 1:
                for way in range(2):
                    lower(owner(way, dist), 2 * dist - 1 + way)
            elif dist == half:
                lower(owner(0, half), fs - 1)

    for k in range(4 * per):
        arrive(k)
        for extra in own_at.get(k, ()):
            send(extra)
        stage(k)

    slots = [(me_f, 0)]
    for dist in range(1, half):
        slots += [(owner(way, dist), 2 * dist - 1 + way) for way in range(2)]
    slots.append((owner(0, half), fs - 1))
    for who, order in slots:
        reduce_wait(recv2, rs2_send, rs2_recv, who, order)
        total_into(out_ref, after, part2, recv2, who)
    for copy in started:
        copy.wait_send()


def on_device(fs, tp, resid, mix_gain, w_query, w_key, w_value, w_gate, w_output, decay_rate,
              mlp_gain, w_up, w_down):
    rows, width = resid.shape
    tokens = rows * tp
    w_in = jnp.concatenate([w_query, w_key, w_value, w_gate], axis=1)
    rates = jnp.broadcast_to(decay_rate[:, None], (decay_rate.shape[0], 128))
    rounds = 4 * (fs - 1)
    vmem = pl.BlockSpec(memory_space=pltpu.VMEM)
    hbm = pl.BlockSpec(memory_space=pl.ANY)
    dma = pltpu.SemaphoreType.DMA
    cols = width // fs
    return pl.pallas_call(
        functools.partial(kernel, fs, tp),
        out_shape=jax.ShapeDtypeStruct((rows, width), BF16),
        in_specs=[vmem] * 4 + [hbm] * 4,
        out_specs=vmem,
        scratch_shapes=[
            pltpu.VMEM((width, w_in.shape[1]), BF16),
            pltpu.VMEM((fs, w_output.shape[0], cols), BF16),
            pltpu.VMEM((width, w_up.shape[1]), BF16),
            pltpu.VMEM((fs, w_down.shape[0], cols), BF16),
            pltpu.VMEM((tokens, width), BF16),
            pltpu.VMEM((tokens, width), BF16),
            pltpu.VMEM((tokens, w_in.shape[1]), BF16),
            pltpu.VMEM((tokens, w_output.shape[0]), BF16),
            pltpu.VMEM((tokens, w_up.shape[1]), BF16),
            pltpu.VMEM((fs, tokens, cols), BF16),
            pltpu.VMEM((tp - 1, fs, rows, cols), BF16),
            pltpu.VMEM((fs, tokens, cols), BF16),
            pltpu.VMEM((tp - 1, fs, rows, cols), BF16),
            pltpu.VMEM((rows, width), BF16),
            dma((2, rounds)),
            dma((2, rounds)),
            dma((4,)),
            dma((2, tp - 1)),
            dma((2, tp - 1)),
            dma((tp - 1, fs)),
            dma((tp - 1, fs)),
            dma((tp - 1, fs)),
            dma((tp - 1, fs)),
        ],
        compiler_params=pltpu.CompilerParams(
            collective_id=0, has_side_effects=True, vmem_limit_bytes=67043328),
    )(resid, mix_gain[None, :], mlp_gain[None, :], rates, w_in, w_output, w_up, w_down)


def solution(mesh):
    placed = (
        P(("fs", "tp"), None),
        P(),
        P("fs", "tp"),
        P("fs", "tp"),
        P("fs", "tp"),
        P("fs", "tp"),
        P("tp", "fs"),
        P("tp"),
        P(),
        P("fs", "tp"),
        P("tp", "fs"),
    )
    sizes = dict(mesh.shape)
    return jax.shard_map(
        functools.partial(on_device, sizes["fs"], sizes["tp"]), mesh=mesh, in_specs=placed,
        out_specs=P(("fs", "tp"), None), check_vma=False)
```

```python
import functools

import jax
import jax.numpy as jnp
from jax import lax
from jax.experimental import pallas as pl
from jax.experimental.pallas import tpu as pltpu
from jax.sharding import PartitionSpec as P

DK = 128
DV = 256
LENGTH = 512
MESH = pl.DeviceIdType.MESH
EPS = 1e-06
F32 = jnp.float32
BF16 = jnp.bfloat16


def tile_of(width):
    return 256 if width % 256 == 0 else 128


def kernel(fs, tp, resid_ref, mix_gain_ref, mlp_gain_ref, rate_ref, wq_ref, wo_ref, wu_ref, wd_ref,
           out_ref, wq, wo, wu, wd, xn, xn2, proj, gated, hidden, part1, core1, chip1, part2, chip2,
           after, ring_send, ring_recv, own_sem, ag_send, ag_recv, line_send, line_recv,
           swap_send, swap_recv, core1_send, core1_recv, chip1_send, chip1_recv, all_send, all_recv,
           core2_send, core2_recv, chip2_send, chip2_recv):
    half = fs // 2
    lines = fs // 2
    chips = tp // 2
    rows = resid_ref.shape[0]
    heads = rate_ref.shape[0]
    tokens = rows * tp
    me_f = lax.axis_index("fs")
    me_t = lax.axis_index("tp")
    pair = me_f % 2
    line = me_f // 2
    other_f = 2 * line + 1 - pair
    chip = me_t // 2
    core = me_t % 2
    other_t = 2 * chip + 1 - core

    def place(i):
        col = i % 2
        at = i // 2
        return at * (1 - col) + (fs - 1 - at) * col

    def index(p):
        col = p // half
        return 2 * (p * (1 - col) + (fs - 1 - p) * col) + col

    my_place = place(me_f)
    target = (index((my_place + 1) % fs), index((my_place + fs - 1) % fs))

    def owner(way, dist):
        if way == 0:
            return index((my_place + fs - dist) % fs)
        return index((my_place + dist) % fs)

    def peer(d):
        return (me_t + d) % tp

    def beside(e):
        return 2 * ((chip + e) % chips) + core

    def step_to(way):
        return me_f + 2 if way == 0 else me_f - 2

    def line_has(way, dist):
        return line >= dist if way == 0 else line + dist <= lines - 1

    def line_next(way):
        return line_has(1 - way, 1)

    barrier = pltpu.get_barrier_semaphore()

    def greet(where):
        pl.semaphore_signal(barrier, inc=1, device_id=where, device_id_type=MESH)

    for way in range(2):
        greet((target[way], me_t))
    for d in range(1, tp):
        greet((me_f, peer(d)))
        if d % 2 == 0:
            greet((other_f, peer(d)))
    greet((other_f, me_t))
    for way in range(2):
        at = (line + (1 if way == 0 else lines - 1)) % lines
        greet((2 * at + pair, me_t))
    pl.semaphore_wait(barrier, 2 + (tp - 1) + (chips - 1) + 1 + 2)

    groups = ((wq_ref, wq, False), (wo_ref, wo, True))
    started = []

    def go(copy, on=None):
        if on is None:
            copy.start()
        else:
            @pl.when(on)
            def _():
                copy.start()
        started.append((copy, on))

    def remote(src, dst, s_sem, r_sem, where):
        return pltpu.make_async_remote_copy(
            src_ref=src, dst_ref=dst, send_sem=s_sem, recv_sem=r_sem, device_id=where,
            device_id_type=MESH)

    def landed(dst, s_sem, r_sem):
        return remote(dst, dst, s_sem, r_sem, (me_f, other_t))

    def span(at, size):
        return pl.ds(pl.multiple_of(at, size), size)

    def slot(w, who, h):
        source, whole, slotted = groups[w]
        deep = source.shape[0]
        hr = deep // 2
        if slotted:
            return whole.at[who, pl.ds(h * hr, hr), :]
        return whole.at[pl.ds(pl.multiple_of(who * deep + h * hr, hr), hr), :]

    rounds = []
    for w in range(2):
        for dist in range(1, half):
            rounds += [(w, dist, 0), (w, dist, 1)]
        rounds.append((w, half, 0))
    per = fs - 1

    def half_of(way, turn):
        return turn if way == 0 else 1 - turn

    def send(k):
        w, dist, turn = rounds[k]
        for way in range(2):
            h = half_of(way, turn)
            who = owner(way, dist - 1)
            source = groups[w][0]
            hr = source.shape[0] // 2
            src = source.at[pl.ds(h * hr, hr), :] if dist == 1 else slot(w, who, h)
            go(remote(src, slot(w, who, h), ring_send.at[way, k], ring_recv.at[way, k],
                      (target[way], me_t)))

    def arrive(k):
        w, dist, turn = rounds[k]
        for way in range(2):
            here = slot(w, owner(way, dist), half_of(way, turn))
            landed(here, ring_send.at[way, k], ring_recv.at[way, k]).wait_recv()
        if dist + 1 < half or (dist + 1 == half and turn == 0):
            send(k + 2)

    up_cols = wu.shape[1]
    deep = wu_ref.shape[0]
    down_rows = wd.shape[1]

    def piece(g, who):
        return wu.at[span(who * deep, deep), :] if g == 0 else wd.at[who]

    def share(g, y):
        if g == 0:
            return wu_ref.at[:, span(y * up_cols, up_cols)]
        return wd_ref.at[span(y * down_rows, down_rows), :]

    def swap_start(g):
        go(remote(share(g, 1 - pair), piece(g, me_f), swap_send.at[g], swap_recv.at[g],
                  (other_f, me_t)))

    def swap_wait(g):
        landed(piece(g, other_f), swap_send.at[g], swap_recv.at[g]).wait_recv()

    line_rounds = [(g, dist, turn) for g in range(2) for dist in range(1, lines) for turn in range(2)]
    per_line = 2 * (lines - 1)

    def line_owner(way, dist, turn):
        at = line - dist if way == 0 else line + dist
        return 2 * at + (pair if turn == 0 else 1 - pair)

    def line_send_round(m, ways=(0, 1)):
        g, dist, turn = line_rounds[m]
        for way in ways:
            who = line_owner(way, dist - 1, turn)
            src = share(g, pair) if dist == 1 and turn == 0 else piece(g, who)
            on = line_next(way) if dist == 1 else jnp.logical_and(line_next(way), line_has(way, dist - 1))
            go(remote(src, piece(g, who), line_send.at[way, m], line_recv.at[way, m],
                      (step_to(way), me_t)), on)

    def line_arrive(m):
        g, dist, turn = line_rounds[m]
        for way in range(2):
            copy = landed(piece(g, line_owner(way, dist, turn)), line_send.at[way, m],
                          line_recv.at[way, m])

            @pl.when(line_has(way, dist))
            def _():
                copy.wait_recv()
            if dist + 1 < lines:
                line_send_round(m + 2, (way,))

    send(0)
    send(1)
    own = []
    for n, (src, dst) in enumerate((
            (wq_ref, wq.at[span(me_f * wq_ref.shape[0], wq_ref.shape[0]), :]),
            (wo_ref, wo.at[me_f]),
            (share(0, pair), piece(0, me_f)),
            (share(1, pair), piece(1, me_f)))):
        copy = pltpu.make_async_copy(src, dst, own_sem.at[n])
        own.append(copy)
    own[0].start()

    my_rows = span(me_t * rows, rows)

    def norm(source, gain_ref):
        wide = source.astype(F32)
        mean = jnp.mean(wide * wide, axis=-1, keepdims=True)
        return (wide * lax.rsqrt(mean + EPS) * gain_ref[...]).astype(BF16)

    step = 64

    def norm_into(buf, first, source_ref, gain_ref):
        @pl.loop(0, rows // step)
        def _(i):
            at = pl.multiple_of(i * step, step)
            buf[pl.ds(pl.multiple_of(first + at, step), step), :] = norm(
                source_ref[pl.ds(at, step), :], gain_ref)

    def ag_block(t):
        return xn.at[span(t * rows, rows), :]

    ag_copies = [remote(ag_block(me_t), ag_block(me_t), ag_send.at[d - 1], ag_recv.at[d - 1],
                        (me_f, peer(d))) for d in range(1, tp)]

    def ag_start():
        for copy in ag_copies:
            copy.start()

    def ag_wait():
        for d in range(1, tp):
            landed(ag_block(peer(tp - d)), ag_send.at[d - 1], ag_recv.at[d - 1]).wait_recv()

    def project():
        width = proj.shape[1]
        t = tile_of(width)

        @pl.loop(0, width // t)
        def _(j):
            cols = pl.ds(pl.multiple_of(j * t, t), t)
            proj[:, cols] = jnp.dot(xn[...], wq[:, cols], preferred_element_type=F32).astype(BF16)

    def retain():
        kq = heads * DK
        vq = heads * DV
        count = tokens // LENGTH
        for head in range(heads):
            rate = rate_ref[head:head + 1, 0:1]

            @pl.loop(0, count)
            def _(n):
                base = pl.multiple_of(n * LENGTH, LENGTH)
                rs = pl.ds(base, LENGTH)
                q = proj[rs, head * DK:(head + 1) * DK]
                k = proj[rs, kq + head * DK:kq + (head + 1) * DK]
                v = proj[rs, 2 * kq + head * DV:2 * kq + (head + 1) * DV]
                g = proj[rs, 2 * kq + vq + head * DV:2 * kq + vq + (head + 1) * DV].astype(F32)
                scores = lax.dot_general(q, k, (((1,), (1,)), ((), ())), preferred_element_type=F32)
                t_at = lax.broadcasted_iota(jnp.int32, (LENGTH, LENGTH), 0)
                s_at = lax.broadcasted_iota(jnp.int32, (LENGTH, LENGTH), 1)
                gap = t_at - s_at
                decay = jnp.exp(-rate * jnp.maximum(gap, 0).astype(F32)) * (DK ** -0.5)
                scores = jnp.where(gap >= 0, scores * decay, 0.0).astype(BF16)
                mixed = jnp.dot(scores, v, preferred_element_type=F32)
                mean = jnp.mean(mixed, axis=-1, keepdims=True)
                off = mixed - mean
                var = jnp.mean(off * off, axis=-1, keepdims=True)
                grouped = off * lax.rsqrt(var + EPS)
                gated[rs, head * DV:(head + 1) * DV] = (g / (1.0 + jnp.exp(-g)) * grouped).astype(BF16)

    def mix_block(x, c):
        return part1.at[span((2 * x + c) * rows, rows), :]

    def mix_out():
        cols = wo.shape[2]

        @pl.loop(0, fs)
        def _(j):
            part1[:, span(j * cols, cols)] = jnp.dot(
                gated[...], wo[j], preferred_element_type=F32).astype(BF16)
        order = [e % chips for e in range(1, chips + 1)]
        for e in order:
            x = (chip + e) % chips
            go(remote(mix_block(x, 1 - core), core1.at[e], core1_send.at[e], core1_recv.at[e],
                      (me_f, other_t)))
        for e in order:
            landed(core1.at[e], core1_send.at[e], core1_recv.at[e]).wait_recv()
            if e:
                first = beside(e) * rows

                @pl.loop(0, rows // step)
                def _(i):
                    at = pl.ds(pl.multiple_of(first + i * step, step), step)
                    more = core1[e, span(i * step, step), :].astype(F32)
                    part1[at, :] = (part1[at, :].astype(F32) + more).astype(BF16)
                go(remote(ag_mix(beside(e)), chip1.at[e - 1], chip1_send.at[e - 1],
                          chip1_recv.at[e - 1], (me_f, beside(e))))

    def ag_mix(t):
        return part1.at[span(t * rows, rows), :]

    def mix_end():
        for e in range(1, chips):
            landed(chip1.at[e - 1], chip1_send.at[e - 1], chip1_recv.at[e - 1]).wait_recv()

        @pl.loop(0, rows // step)
        def _(i):
            at = span(i * step, step)
            total = part1[pl.ds(pl.multiple_of(me_t * rows + i * step, step), step), :].astype(F32)
            total = total + core1[0, at, :].astype(F32)
            for e in range(1, chips):
                total = total + chip1[e - 1, at, :].astype(F32)
            sum_ = (resid_ref[at, :].astype(F32) + total).astype(BF16)
            after[at, :] = sum_
            xn2[pl.ds(pl.multiple_of(block(pair, me_t) * rows + i * step, step), step), :] = norm(
                sum_, mlp_gain_ref)

    def block(y, t):
        return (t % 2) * (2 * chips) + y * chips + t // 2

    def wide(y, t, part=None):
        first = block(y, t) * rows
        hr = rows // 2
        if part is None:
            return xn2.at[span(first, rows), :]
        return xn2.at[pl.ds(pl.multiple_of(first + part * hr, hr), hr), :]

    more_chips = chips - 1
    pieces = 1 + 3 * more_chips

    def all_copy(n, ref, where):
        go(remote(ref, ref, all_send.at[n], all_recv.at[n], where))

    def all_landed(n, ref):
        landed(ref, all_send.at[n], all_recv.at[n]).wait_recv()

    def across(n, ref):
        all_copy(pieces + n, ref, (me_f, other_t))

    def all_first():
        ref = wide(pair, me_t)
        all_copy(0, ref, (other_f, me_t))
        for e in range(1, chips):
            all_copy(e, ref, (me_f, beside(e)))
        all_copy(2 * pieces, ref, (me_f, other_t))

    def all_second():
        ref = wide(1 - pair, me_t)
        all_landed(0, ref)
        for e in range(1, chips):
            all_copy(more_chips + e, wide(1 - pair, me_t, 0), (me_f, beside(e)))
        across(0, ref)
        for e in range(1, chips):
            t = beside(chips - e)
            all_landed(e, wide(pair, t))
            all_copy(2 * more_chips + e, wide(pair, t, 1), (other_f, me_t))
            across(e, wide(pair, t))

    def all_third():
        for part in range(2):
            for e in range(1, chips):
                n = (1 + part) * more_chips + e
                ref = wide(1 - pair, beside(chips - e), part)
                all_landed(n, ref)
                across(n, ref)
        all_landed(2 * pieces, wide(pair, other_t))
        all_landed(pieces, wide(1 - pair, other_t))
        for e in range(1, chips):
            t = 2 * ((chip + chips - e) % chips) + 1 - core
            all_landed(pieces + e, wide(pair, t))
            for part in range(2):
                all_landed(pieces + (1 + part) * more_chips + e, wide(1 - pair, t, part))

    def lift():
        t = tile_of(up_cols)

        @pl.loop(0, 2)
        def _(i):
            at = span(i * tokens, tokens)

            @pl.loop(0, up_cols // t)
            def _(j):
                cols = span(j * t, t)
                up = jnp.maximum(jnp.dot(xn2[at, :], wu[:, cols], preferred_element_type=F32), 0.0)
                hidden[at, cols] = (up * up).astype(BF16)

    cw = wd.shape[2]
    r2 = 2 * chips - 1

    def mlp_copies(who):
        cols = span(who * cw, cw)
        first = core * tokens
        side = remote(part2.at[span((1 - core) * tokens, tokens), cols], xn.at[:, cols],
                      core2_send.at[who], core2_recv.at[who], (me_f, other_t))
        side_in = landed(xn.at[:, cols], core2_send.at[who], core2_recv.at[who])
        outs, ins = [], []
        n = 0
        for dy in range(2):
            for e in range(chips):
                if dy == 0 and e == 0:
                    continue
                y = pair if dy == 0 else 1 - pair
                t = beside(e)
                dst = chip2.at[n, :, cols]
                outs.append(remote(part2.at[span(block(y, t) * rows, rows), cols], dst,
                                   chip2_send.at[n, who], chip2_recv.at[n, who],
                                   (me_f if dy == 0 else other_f, t)))
                ins.append(landed(dst, chip2_send.at[n, who], chip2_recv.at[n, who]))
                n += 1
        return side, side_in, outs, ins

    finals = []

    def lower(who, on=None):
        side, side_in, outs, ins = mlp_copies(who)
        cols = span(who * cw, cw)
        mine = block(pair, me_t) * rows

        def run():
            @pl.loop(0, 2)
            def _(i):
                at = span(((1 - core) * (1 - i) + core * i) * tokens, tokens)
                part2[at, cols] = jnp.dot(
                    hidden[at, :], wd[who], preferred_element_type=F32).astype(BF16)

                @pl.when(i == 0)
                def _():
                    side.start()
            side_in.wait_recv()

            @pl.loop(0, tokens // 128)
            def _(i):
                at = pl.ds(pl.multiple_of(core * tokens + i * 128, 128), 128)
                more = xn[span(i * 128, 128), cols].astype(F32)
                part2[at, cols] = (part2[at, cols].astype(F32) + more).astype(BF16)
            for copy in outs:
                copy.start()

        def end():
            for copy in ins:
                copy.wait_recv()
            total = part2[span(mine, rows), cols].astype(F32)
            for n in range(r2):
                total = total + chip2[n, :, cols].astype(F32)
            out_ref[:, cols] = (after[:, cols].astype(F32) + total).astype(BF16)
            side.wait_send()
            for copy in outs:
                copy.wait_send()

        if on is None:
            run()
        else:
            pl.when(on)(run)
        finals.append((end, on))

    norm_into(xn, me_t * rows, resid_ref, mix_gain_ref)
    ag_start()
    for copy in own[1:]:
        copy.start()

    own_at = {per - 3: [per], per - 2: [per + 1]}

    for k in range(2 * per):
        arrive(k)
        for extra in own_at.get(k, ()):
            send(extra)
        if k == per - 1:
            line_send_round(0)
            own[0].wait()
            ag_wait()
            project()
        elif k == per:
            swap_start(0)
        elif k == per + 1:
            retain()
        elif k == 2 * per - 2:
            swap_wait(0)
            line_send_round(1)
            swap_start(1)
        elif k == 2 * per - 1:
            own[1].wait()
            mix_out()

    last_d = per_line - 2
    for m in range(2 * per_line):
        line_arrive(m)
        if m == last_d - 1:
            line_send_round(per_line)
        elif m == last_d:
            swap_wait(1)
            line_send_round(per_line + 1)
        if m == max(per_line - 4, 0):
            for copy in ag_copies:
                copy.wait_send()
            mix_end()
            all_first()
        elif m == per_line - 1:
            all_second()
        elif m == per_line:
            own[2].wait()
            own[3].wait()
            all_third()
            lift()
            lower(me_f)
            lower(other_f)
        if m >= per_line:
            _, dist, turn = line_rounds[m]
            for way in range(2):
                lower(line_owner(way, dist, turn), line_has(way, dist))

    for end, on in finals:
        if on is None:
            end()
        else:
            pl.when(on)(end)
    for copy, on in started:
        if on is None:
            copy.wait_send()
        else:
            pl.when(on)(copy.wait_send)


def on_device(fs, tp, resid, mix_gain, w_query, w_key, w_value, w_gate, w_output, decay_rate,
              mlp_gain, w_up, w_down):
    rows, width = resid.shape
    tokens = rows * tp
    w_in = jnp.concatenate([w_query, w_key, w_value, w_gate], axis=1)
    rates = jnp.broadcast_to(decay_rate[:, None], (decay_rate.shape[0], 128))
    chips = tp // 2
    wide = 2 * (1 + 3 * (chips - 1)) + 1
    vmem = pl.BlockSpec(memory_space=pltpu.VMEM)
    hbm = pl.BlockSpec(memory_space=pl.ANY)
    dma = pltpu.SemaphoreType.DMA
    cols = width // fs
    return pl.pallas_call(
        functools.partial(kernel, fs, tp),
        out_shape=jax.ShapeDtypeStruct((rows, width), BF16),
        in_specs=[vmem] * 4 + [hbm] * 4,
        out_specs=vmem,
        scratch_shapes=[
            pltpu.VMEM((width, w_in.shape[1]), BF16),
            pltpu.VMEM((fs, w_output.shape[0], cols), BF16),
            pltpu.VMEM((width, w_up.shape[1] // 2), BF16),
            pltpu.VMEM((fs, w_down.shape[0] // 2, cols), BF16),
            pltpu.VMEM((tokens, width), BF16),
            pltpu.VMEM((2 * tokens, width), BF16),
            pltpu.VMEM((tokens, w_in.shape[1]), BF16),
            pltpu.VMEM((tokens, w_output.shape[0]), BF16),
            pltpu.VMEM((2 * tokens, w_up.shape[1] // 2), BF16),
            pltpu.VMEM((tokens, width), BF16),
            pltpu.VMEM((chips, rows, width), BF16),
            pltpu.VMEM((chips - 1, rows, width), BF16),
            pltpu.VMEM((2 * tokens, width), BF16),
            pltpu.VMEM((2 * chips - 1, rows, width), BF16),
            pltpu.VMEM((rows, width), BF16),
            dma((2, 2 * (fs - 1))),
            dma((2, 2 * (fs - 1))),
            dma((4,)),
            dma((tp - 1,)),
            dma((tp - 1,)),
            dma((2, 2 * (fs - 2))),
            dma((2, 2 * (fs - 2))),
            dma((2,)),
            dma((2,)),
            dma((chips,)),
            dma((chips,)),
            dma((chips - 1,)),
            dma((chips - 1,)),
            dma((wide,)),
            dma((wide,)),
            dma((fs,)),
            dma((fs,)),
            dma((2 * chips - 1, fs)),
            dma((2 * chips - 1, fs)),
        ],
        compiler_params=pltpu.CompilerParams(
            collective_id=0, has_side_effects=True, vmem_limit_bytes=67043328),
    )(resid, mix_gain[None, :], mlp_gain[None, :], rates, w_in, w_output, w_up, w_down)


def solution(mesh):
    placed = (
        P(("fs", "tp"), None),
        P(),
        P("fs", "tp"),
        P("fs", "tp"),
        P("fs", "tp"),
        P("fs", "tp"),
        P("tp", "fs"),
        P("tp"),
        P(),
        P("fs", "tp"),
        P("tp", "fs"),
    )
    sizes = dict(mesh.shape)
    return jax.shard_map(
        functools.partial(on_device, sizes["fs"], sizes["tp"]), mesh=mesh, in_specs=placed,
        out_specs=P(("fs", "tp"), None), check_vma=False)
```

```python
import functools

import jax
import jax.numpy as jnp
from jax import lax
from jax.experimental import pallas as pl
from jax.experimental.pallas import tpu as pltpu
from jax.sharding import PartitionSpec as P

DK = 128
DV = 256
LENGTH = 512
MESH = pl.DeviceIdType.MESH
EPS = 1e-06
F32 = jnp.float32
BF16 = jnp.bfloat16


def tile_of(width):
    return 256 if width % 256 == 0 else 128


def kernel(fs, tp, resid_ref, mix_gain_ref, mlp_gain_ref, rate_ref, w1_ref, w2_ref, w3_ref, w4_ref, wo_ref, wu_ref, wd_ref,
           out_ref, wq, wo, wu, wd, xn, xn2, proj, gated, hidden, part1, core1, chip1, part2, chip2,
           after, ring_send, ring_recv, own_sem, in_sem, ag_send, ag_recv, line_send, line_recv,
           swap_send, swap_recv, core1_send, core1_recv, chip1_send, chip1_recv, all_send, all_recv,
           core2_send, core2_recv, chip2_send, chip2_recv):
    half = fs // 2
    lines = fs // 2
    in_refs = (w1_ref, w2_ref, w3_ref, w4_ref)
    deep_q = w1_ref.shape[0]
    chips = tp // 2
    rows = resid_ref.shape[0]
    heads = rate_ref.shape[0]
    tokens = rows * tp
    me_f = lax.axis_index("fs")
    me_t = lax.axis_index("tp")
    pair = me_f % 2
    line = me_f // 2
    other_f = 2 * line + 1 - pair
    chip = me_t // 2
    core = me_t % 2
    other_t = 2 * chip + 1 - core

    def place(i):
        col = i % 2
        at = i // 2
        return at * (1 - col) + (fs - 1 - at) * col

    def index(p):
        col = p // half
        return 2 * (p * (1 - col) + (fs - 1 - p) * col) + col

    my_place = place(me_f)
    target = (index((my_place + 1) % fs), index((my_place + fs - 1) % fs))

    def owner(way, dist):
        if way == 0:
            return index((my_place + fs - dist) % fs)
        return index((my_place + dist) % fs)

    def peer(d):
        return (me_t + d) % tp

    def beside(e):
        return 2 * ((chip + e) % chips) + core

    def step_to(way):
        return me_f + 2 if way == 0 else me_f - 2

    def line_has(way, dist):
        return line >= dist if way == 0 else line + dist <= lines - 1

    def line_next(way):
        return line_has(1 - way, 1)

    first_row = pl.multiple_of(me_f * deep_q, deep_q)
    loads = []
    left = 0
    for n, ref in enumerate(in_refs):
        copy = pltpu.make_async_copy(
            ref, wq.at[pl.ds(first_row, deep_q), left:left + ref.shape[1]], in_sem.at[n])
        copy.start()
        loads.append(copy)
        left += ref.shape[1]

    barrier = pltpu.get_barrier_semaphore()

    def greet(where):
        pl.semaphore_signal(barrier, inc=1, device_id=where, device_id_type=MESH)

    for way in range(2):
        greet((target[way], me_t))
    for d in range(1, tp):
        greet((me_f, peer(d)))
        if d % 2 == 0:
            greet((other_f, peer(d)))
    greet((other_f, me_t))
    for way in range(2):
        at = (line + (1 if way == 0 else lines - 1)) % lines
        greet((2 * at + pair, me_t))
    pl.semaphore_wait(barrier, 2 + (tp - 1) + (chips - 1) + 1 + 2)

    groups = ((None, wq, False), (wo_ref, wo, True))
    started = []

    def go(copy, on=None):
        if on is None:
            copy.start()
        else:
            @pl.when(on)
            def _():
                copy.start()
        started.append((copy, on))

    def remote(src, dst, s_sem, r_sem, where):
        return pltpu.make_async_remote_copy(
            src_ref=src, dst_ref=dst, send_sem=s_sem, recv_sem=r_sem, device_id=where,
            device_id_type=MESH)

    def landed(dst, s_sem, r_sem):
        return remote(dst, dst, s_sem, r_sem, (me_f, other_t))

    def span(at, size):
        return pl.ds(pl.multiple_of(at, size), size)

    def slot(w, who, h):
        source, whole, slotted = groups[w]
        hr = (deep_q if w == 0 else source.shape[0]) // 2
        deep = 2 * hr
        if slotted:
            return whole.at[who, pl.ds(h * hr, hr), :]
        return whole.at[pl.ds(pl.multiple_of(who * deep + h * hr, hr), hr), :]

    rounds = []
    for w in range(2):
        for dist in range(1, half):
            rounds += [(w, dist, 0), (w, dist, 1)]
        rounds.append((w, half, 0))
    per = fs - 1

    def half_of(way, turn):
        return turn if way == 0 else 1 - turn

    def send(k):
        w, dist, turn = rounds[k]
        for way in range(2):
            h = half_of(way, turn)
            who = owner(way, dist - 1)
            src = slot(w, who, h)
            if dist == 1 and w == 1:
                hr = wo_ref.shape[0] // 2
                src = wo_ref.at[pl.ds(h * hr, hr), :]
            go(remote(src, slot(w, who, h), ring_send.at[way, k], ring_recv.at[way, k],
                      (target[way], me_t)))

    def arrive(k):
        w, dist, turn = rounds[k]
        for way in range(2):
            here = slot(w, owner(way, dist), half_of(way, turn))
            landed(here, ring_send.at[way, k], ring_recv.at[way, k]).wait_recv()
        if dist + 1 < half or (dist + 1 == half and turn == 0):
            send(k + 2)

    up_cols = wu.shape[1]
    deep = wu_ref.shape[0]
    down_rows = wd.shape[1]

    def piece(g, who):
        return wu.at[span(who * deep, deep), :] if g == 0 else wd.at[who]

    def share(g, y):
        if g == 0:
            return wu_ref.at[:, span(y * up_cols, up_cols)]
        return wd_ref.at[span(y * down_rows, down_rows), :]

    def swap_start(g):
        go(remote(share(g, 1 - pair), piece(g, me_f), swap_send.at[g], swap_recv.at[g],
                  (other_f, me_t)))

    def swap_wait(g):
        landed(piece(g, other_f), swap_send.at[g], swap_recv.at[g]).wait_recv()

    line_rounds = [(g, dist, turn) for g in range(2) for dist in range(1, lines) for turn in range(2)]
    per_line = 2 * (lines - 1)

    def line_owner(way, dist, turn):
        at = line - dist if way == 0 else line + dist
        return 2 * at + (pair if turn == 0 else 1 - pair)

    def line_send_round(m, ways=(0, 1)):
        g, dist, turn = line_rounds[m]
        for way in ways:
            who = line_owner(way, dist - 1, turn)
            src = share(g, pair) if dist == 1 and turn == 0 else piece(g, who)
            on = line_next(way) if dist == 1 else jnp.logical_and(line_next(way), line_has(way, dist - 1))
            go(remote(src, piece(g, who), line_send.at[way, m], line_recv.at[way, m],
                      (step_to(way), me_t)), on)

    def line_arrive(m):
        g, dist, turn = line_rounds[m]
        for way in range(2):
            copy = landed(piece(g, line_owner(way, dist, turn)), line_send.at[way, m],
                          line_recv.at[way, m])

            @pl.when(line_has(way, dist))
            def _():
                copy.wait_recv()
            if dist + 1 < lines:
                line_send_round(m + 2, (way,))

    for copy in loads:
        copy.wait()
    send(0)
    send(1)
    own = [None]
    for n, (src, dst) in enumerate((
            (wo_ref, wo.at[me_f]),
            (share(0, pair), piece(0, me_f)),
            (share(1, pair), piece(1, me_f)))):
        copy = pltpu.make_async_copy(src, dst, own_sem.at[n])
        own.append(copy)

    my_rows = span(me_t * rows, rows)

    def norm(source, gain_ref):
        wide = source.astype(F32)
        mean = jnp.mean(wide * wide, axis=-1, keepdims=True)
        return (wide * lax.rsqrt(mean + EPS) * gain_ref[...]).astype(BF16)

    step = 64

    def norm_into(buf, first, source_ref, gain_ref):
        @pl.loop(0, rows // step)
        def _(i):
            at = pl.multiple_of(i * step, step)
            buf[pl.ds(pl.multiple_of(first + at, step), step), :] = norm(
                source_ref[pl.ds(at, step), :], gain_ref)

    def ag_block(t):
        return xn.at[span(t * rows, rows), :]

    ag_copies = [remote(ag_block(me_t), ag_block(me_t), ag_send.at[d - 1], ag_recv.at[d - 1],
                        (me_f, peer(d))) for d in range(1, tp)]

    def ag_start():
        for copy in ag_copies:
            copy.start()

    def ag_wait():
        for d in range(1, tp):
            landed(ag_block(peer(tp - d)), ag_send.at[d - 1], ag_recv.at[d - 1]).wait_recv()

    def project():
        width = proj.shape[1]
        t = tile_of(width)

        @pl.loop(0, width // t)
        def _(j):
            cols = pl.ds(pl.multiple_of(j * t, t), t)
            proj[:, cols] = jnp.dot(xn[...], wq[:, cols], preferred_element_type=F32).astype(BF16)

    def retain():
        kq = heads * DK
        vq = heads * DV
        count = tokens // LENGTH
        for head in range(heads):
            rate = rate_ref[head]

            @pl.loop(0, count)
            def _(n):
                base = pl.multiple_of(n * LENGTH, LENGTH)
                rs = pl.ds(base, LENGTH)
                q = proj[rs, head * DK:(head + 1) * DK]
                k = proj[rs, kq + head * DK:kq + (head + 1) * DK]
                v = proj[rs, 2 * kq + head * DV:2 * kq + (head + 1) * DV]
                g = proj[rs, 2 * kq + vq + head * DV:2 * kq + vq + (head + 1) * DV].astype(F32)
                scores = lax.dot_general(q, k, (((1,), (1,)), ((), ())), preferred_element_type=F32)
                t_at = lax.broadcasted_iota(jnp.int32, (LENGTH, LENGTH), 0)
                s_at = lax.broadcasted_iota(jnp.int32, (LENGTH, LENGTH), 1)
                gap = t_at - s_at
                decay = jnp.exp(-rate * jnp.maximum(gap, 0).astype(F32)) * (DK ** -0.5)
                scores = jnp.where(gap >= 0, scores * decay, 0.0).astype(BF16)
                mixed = jnp.dot(scores, v, preferred_element_type=F32)
                mean = jnp.mean(mixed, axis=-1, keepdims=True)
                off = mixed - mean
                var = jnp.mean(off * off, axis=-1, keepdims=True)
                grouped = off * lax.rsqrt(var + EPS)
                gated[rs, head * DV:(head + 1) * DV] = (g / (1.0 + jnp.exp(-g)) * grouped).astype(BF16)

    def mix_block(x, c):
        return part1.at[span((2 * x + c) * rows, rows), :]

    def mix_out():
        cols = wo.shape[2]

        @pl.loop(0, fs)
        def _(j):
            part1[:, span(j * cols, cols)] = jnp.dot(
                gated[...], wo[j], preferred_element_type=F32).astype(BF16)
        order = [e % chips for e in range(1, chips + 1)]
        for e in order:
            x = (chip + e) % chips
            go(remote(mix_block(x, 1 - core), core1.at[e], core1_send.at[e], core1_recv.at[e],
                      (me_f, other_t)))
        for e in order:
            landed(core1.at[e], core1_send.at[e], core1_recv.at[e]).wait_recv()
            if e:
                first = beside(e) * rows

                @pl.loop(0, rows // step)
                def _(i):
                    at = pl.ds(pl.multiple_of(first + i * step, step), step)
                    more = core1[e, span(i * step, step), :].astype(F32)
                    part1[at, :] = (part1[at, :].astype(F32) + more).astype(BF16)
                go(remote(ag_mix(beside(e)), chip1.at[e - 1], chip1_send.at[e - 1],
                          chip1_recv.at[e - 1], (me_f, beside(e))))

    def ag_mix(t):
        return part1.at[span(t * rows, rows), :]

    def mix_end():
        for e in range(1, chips):
            landed(chip1.at[e - 1], chip1_send.at[e - 1], chip1_recv.at[e - 1]).wait_recv()

        @pl.loop(0, rows // step)
        def _(i):
            at = span(i * step, step)
            total = part1[pl.ds(pl.multiple_of(me_t * rows + i * step, step), step), :].astype(F32)
            total = total + core1[0, at, :].astype(F32)
            for e in range(1, chips):
                total = total + chip1[e - 1, at, :].astype(F32)
            sum_ = (resid_ref[at, :].astype(F32) + total).astype(BF16)
            after[at, :] = sum_
            xn2[pl.ds(pl.multiple_of(block(pair, me_t) * rows + i * step, step), step), :] = norm(
                sum_, mlp_gain_ref)

    def block(y, t):
        return (t % 2) * (2 * chips) + y * chips + t // 2

    def wide(y, t, part=None):
        first = block(y, t) * rows
        hr = rows // 2
        if part is None:
            return xn2.at[span(first, rows), :]
        return xn2.at[pl.ds(pl.multiple_of(first + part * hr, hr), hr), :]

    more_chips = chips - 1
    pieces = 1 + 3 * more_chips

    def all_copy(n, ref, where):
        go(remote(ref, ref, all_send.at[n], all_recv.at[n], where))

    def all_landed(n, ref):
        landed(ref, all_send.at[n], all_recv.at[n]).wait_recv()

    def across(n, ref):
        all_copy(pieces + n, ref, (me_f, other_t))

    def all_first():
        ref = wide(pair, me_t)
        all_copy(0, ref, (other_f, me_t))
        for e in range(1, chips):
            all_copy(e, ref, (me_f, beside(e)))
        all_copy(2 * pieces, ref, (me_f, other_t))

    def all_second():
        ref = wide(1 - pair, me_t)
        all_landed(0, ref)
        for e in range(1, chips):
            all_copy(more_chips + e, wide(1 - pair, me_t, 0), (me_f, beside(e)))
        across(0, ref)
        for e in range(1, chips):
            t = beside(chips - e)
            all_landed(e, wide(pair, t))
            all_copy(2 * more_chips + e, wide(pair, t, 1), (other_f, me_t))
            across(e, wide(pair, t))

    def all_third():
        for part in range(2):
            for e in range(1, chips):
                n = (1 + part) * more_chips + e
                ref = wide(1 - pair, beside(chips - e), part)
                all_landed(n, ref)
                across(n, ref)
        all_landed(2 * pieces, wide(pair, other_t))
        all_landed(pieces, wide(1 - pair, other_t))
        for e in range(1, chips):
            t = 2 * ((chip + chips - e) % chips) + 1 - core
            all_landed(pieces + e, wide(pair, t))
            for part in range(2):
                all_landed(pieces + (1 + part) * more_chips + e, wide(1 - pair, t, part))

    def lift():
        t = tile_of(up_cols)

        @pl.loop(0, 2)
        def _(i):
            at = span(i * tokens, tokens)

            @pl.loop(0, up_cols // t)
            def _(j):
                cols = span(j * t, t)
                up = jnp.maximum(jnp.dot(xn2[at, :], wu[:, cols], preferred_element_type=F32), 0.0)
                hidden[at, cols] = (up * up).astype(BF16)

    cw = wd.shape[2]
    r2 = 2 * chips - 1

    def mlp_copies(who):
        cols = span(who * cw, cw)
        first = core * tokens
        side = remote(part2.at[span((1 - core) * tokens, tokens), cols], xn.at[:, cols],
                      core2_send.at[who], core2_recv.at[who], (me_f, other_t))
        side_in = landed(xn.at[:, cols], core2_send.at[who], core2_recv.at[who])
        outs, ins = [], []
        n = 0
        for dy in range(2):
            for e in range(chips):
                if dy == 0 and e == 0:
                    continue
                y = pair if dy == 0 else 1 - pair
                t = beside(e)
                dst = chip2.at[n, :, cols]
                outs.append(remote(part2.at[span(block(y, t) * rows, rows), cols], dst,
                                   chip2_send.at[n, who], chip2_recv.at[n, who],
                                   (me_f if dy == 0 else other_f, t)))
                ins.append(landed(dst, chip2_send.at[n, who], chip2_recv.at[n, who]))
                n += 1
        return side, side_in, outs, ins

    finals = []

    def lower(who, on=None):
        side, side_in, outs, ins = mlp_copies(who)
        cols = span(who * cw, cw)
        mine = block(pair, me_t) * rows

        def run():
            @pl.loop(0, 2)
            def _(i):
                at = span(((1 - core) * (1 - i) + core * i) * tokens, tokens)
                part2[at, cols] = jnp.dot(
                    hidden[at, :], wd[who], preferred_element_type=F32).astype(BF16)

                @pl.when(i == 0)
                def _():
                    side.start()
            side_in.wait_recv()

            @pl.loop(0, tokens // 128)
            def _(i):
                at = pl.ds(pl.multiple_of(core * tokens + i * 128, 128), 128)
                more = xn[span(i * 128, 128), cols].astype(F32)
                part2[at, cols] = (part2[at, cols].astype(F32) + more).astype(BF16)
            for copy in outs:
                copy.start()

        def end():
            for copy in ins:
                copy.wait_recv()
            total = part2[span(mine, rows), cols].astype(F32)
            for n in range(r2):
                total = total + chip2[n, :, cols].astype(F32)
            out_ref[:, cols] = (after[:, cols].astype(F32) + total).astype(BF16)
            side.wait_send()
            for copy in outs:
                copy.wait_send()

        if on is None:
            run()
        else:
            pl.when(on)(run)
        finals.append((end, on))

    norm_into(xn, me_t * rows, resid_ref, mix_gain_ref)
    ag_start()
    for copy in own[1:]:
        copy.start()

    own_at = {per - 3: [per], per - 2: [per + 1]}

    for k in range(2 * per):
        arrive(k)
        for extra in own_at.get(k, ()):
            send(extra)
        if k == per - 1:
            line_send_round(0)
            ag_wait()
            project()
        elif k == per:
            swap_start(0)
        elif k == per + 1:
            retain()
        elif k == 2 * per - 2:
            swap_wait(0)
            line_send_round(1)
            swap_start(1)
        elif k == 2 * per - 1:
            own[1].wait()
            mix_out()

    last_d = per_line - 2
    for m in range(2 * per_line):
        line_arrive(m)
        if m == last_d - 1:
            line_send_round(per_line)
        elif m == last_d:
            swap_wait(1)
            line_send_round(per_line + 1)
        if m == per_line + (-3):
            for copy in ag_copies:
                copy.wait_send()
            mix_end()
            all_first()
        elif m == per_line + (-1):
            all_second()
        elif m == per_line:
            own[2].wait()
            own[3].wait()
            all_third()
            lift()
            lower(me_f)
            lower(other_f)
        if m >= per_line:
            _, dist, turn = line_rounds[m]
            for way in range(2):
                lower(line_owner(way, dist, turn), line_has(way, dist))

    for end, on in finals:
        if on is None:
            end()
        else:
            pl.when(on)(end)
    for copy, on in started:
        if on is None:
            copy.wait_send()
        else:
            pl.when(on)(copy.wait_send)


def on_device(fs, tp, resid, mix_gain, w_query, w_key, w_value, w_gate, w_output, decay_rate,
              mlp_gain, w_up, w_down):
    rows, width = resid.shape
    tokens = rows * tp
    in_width = w_query.shape[1] + w_key.shape[1] + w_value.shape[1] + w_gate.shape[1]
    chips = tp // 2
    wide = 2 * (1 + 3 * (chips - 1)) + 1
    vmem = pl.BlockSpec(memory_space=pltpu.VMEM)
    hbm = pl.BlockSpec(memory_space=pl.ANY)
    dma = pltpu.SemaphoreType.DMA
    cols = width // fs
    return pl.pallas_call(
        functools.partial(kernel, fs, tp),
        out_shape=jax.ShapeDtypeStruct((rows, width), BF16),
        in_specs=[vmem] * 3 + [pl.BlockSpec(memory_space=pltpu.SMEM)] + [hbm] * 7,
        out_specs=vmem,
        scratch_shapes=[
            pltpu.VMEM((width, in_width), BF16),
            pltpu.VMEM((fs, w_output.shape[0], cols), BF16),
            pltpu.VMEM((width, w_up.shape[1] // 2), BF16),
            pltpu.VMEM((fs, w_down.shape[0] // 2, cols), BF16),
            pltpu.VMEM((tokens, width), BF16),
            pltpu.VMEM((2 * tokens, width), BF16),
            pltpu.VMEM((tokens, in_width), BF16),
            pltpu.VMEM((tokens, w_output.shape[0]), BF16),
            pltpu.VMEM((2 * tokens, w_up.shape[1] // 2), BF16),
            pltpu.VMEM((tokens, width), BF16),
            pltpu.VMEM((chips, rows, width), BF16),
            pltpu.VMEM((chips - 1, rows, width), BF16),
            pltpu.VMEM((2 * tokens, width), BF16),
            pltpu.VMEM((2 * chips - 1, rows, width), BF16),
            pltpu.VMEM((rows, width), BF16),
            dma((2, 2 * (fs - 1))),
            dma((2, 2 * (fs - 1))),
            dma((3,)),
            dma((4,)),
            dma((tp - 1,)),
            dma((tp - 1,)),
            dma((2, 2 * (fs - 2))),
            dma((2, 2 * (fs - 2))),
            dma((2,)),
            dma((2,)),
            dma((chips,)),
            dma((chips,)),
            dma((chips - 1,)),
            dma((chips - 1,)),
            dma((wide,)),
            dma((wide,)),
            dma((fs,)),
            dma((fs,)),
            dma((2 * chips - 1, fs)),
            dma((2 * chips - 1, fs)),
        ],
        compiler_params=pltpu.CompilerParams(
            collective_id=0, has_side_effects=True, vmem_limit_bytes=67043328),
    )(resid, mix_gain[None, :], mlp_gain[None, :], decay_rate, w_query, w_key, w_value,
      w_gate, w_output, w_up, w_down)


def solution(mesh):
    placed = (
        P(("fs", "tp"), None),
        P(),
        P("fs", "tp"),
        P("fs", "tp"),
        P("fs", "tp"),
        P("fs", "tp"),
        P("tp", "fs"),
        P("tp"),
        P(),
        P("fs", "tp"),
        P("tp", "fs"),
    )
    sizes = dict(mesh.shape)
    return jax.shard_map(
        functools.partial(on_device, sizes["fs"], sizes["tp"]), mesh=mesh, in_specs=placed,
        out_specs=P(("fs", "tp"), None), check_vma=False)
```

```python
import functools

import jax
import jax.numpy as jnp
from jax import lax
from jax.experimental import pallas as pl
from jax.experimental.pallas import tpu as pltpu
from jax.sharding import PartitionSpec as P

DK = 128
DV = 256
LENGTH = 512
MESH = pl.DeviceIdType.MESH
EPS = 1e-06
F32 = jnp.float32
BF16 = jnp.bfloat16


def tile_of(width):
    return 256 if width % 256 == 0 else 128


def kernel(fs, tp, resid_ref, mix_gain_ref, mlp_gain_ref, rate_ref, w1_ref, w2_ref, w3_ref, w4_ref, wo_ref, wu_ref, wd_ref,
           out_ref, wq, wo, wu, wd, xn, xn2, proj, gated, hidden, part1, core1, chip1, part2, chip2,
           after, ring_send, ring_recv, own_sem, in_sem, ag_send, ag_recv, line_send, line_recv,
           swap_send, swap_recv, core1_send, core1_recv, chip1_send, chip1_recv, all_send, all_recv,
           core2_send, core2_recv, chip2_send, chip2_recv):
    half = fs // 2
    lines = fs // 2
    in_refs = (w1_ref, w2_ref, w3_ref, w4_ref)
    deep_q = w1_ref.shape[0]
    chips = tp // 2
    rows = resid_ref.shape[0]
    heads = rate_ref.shape[0]
    tokens = rows * tp
    me_f = lax.axis_index("fs")
    me_t = lax.axis_index("tp")
    pair = me_f % 2
    line = me_f // 2
    other_f = 2 * line + 1 - pair
    chip = me_t // 2
    core = me_t % 2
    other_t = 2 * chip + 1 - core

    def place(i):
        col = i % 2
        at = i // 2
        return at * (1 - col) + (fs - 1 - at) * col

    def index(p):
        col = p // half
        return 2 * (p * (1 - col) + (fs - 1 - p) * col) + col

    my_place = place(me_f)
    target = (index((my_place + 1) % fs), index((my_place + fs - 1) % fs))

    def owner(way, dist):
        if way == 0:
            return index((my_place + fs - dist) % fs)
        return index((my_place + dist) % fs)

    def peer(d):
        return (me_t + d) % tp

    def beside(e):
        return 2 * ((chip + e) % chips) + core

    def step_to(way):
        return me_f + 2 if way == 0 else me_f - 2

    def line_has(way, dist):
        return line >= dist if way == 0 else line + dist <= lines - 1

    def line_next(way):
        return line_has(1 - way, 1)

    first_row = pl.multiple_of(me_f * deep_q, deep_q)
    loads = []
    left = 0
    for n, ref in enumerate(in_refs):
        copy = pltpu.make_async_copy(
            ref, wq.at[pl.ds(first_row, deep_q), left:left + ref.shape[1]], in_sem.at[n])
        copy.start()
        loads.append(copy)
        left += ref.shape[1]

    barrier = pltpu.get_barrier_semaphore()

    def greet(where):
        pl.semaphore_signal(barrier, inc=1, device_id=where, device_id_type=MESH)

    for way in range(2):
        greet((target[way], me_t))
    for d in range(1, tp):
        greet((me_f, peer(d)))
        if d % 2 == 0:
            greet((other_f, peer(d)))
    greet((other_f, me_t))
    for way in range(2):
        at = (line + (1 if way == 0 else lines - 1)) % lines
        greet((2 * at + pair, me_t))
    pl.semaphore_wait(barrier, 2 + (tp - 1) + (chips - 1) + 1 + 2)

    groups = ((None, wq, False), (wo_ref, wo, True))
    started = []

    def go(copy, on=None):
        if on is None:
            copy.start()
        else:
            @pl.when(on)
            def _():
                copy.start()
        started.append((copy, on))

    def remote(src, dst, s_sem, r_sem, where):
        return pltpu.make_async_remote_copy(
            src_ref=src, dst_ref=dst, send_sem=s_sem, recv_sem=r_sem, device_id=where,
            device_id_type=MESH)

    def landed(dst, s_sem, r_sem):
        return remote(dst, dst, s_sem, r_sem, (me_f, other_t))

    def span(at, size):
        return pl.ds(pl.multiple_of(at, size), size)

    def slot(w, who, h):
        source, whole, slotted = groups[w]
        hr = (deep_q if w == 0 else source.shape[0]) // 2
        deep = 2 * hr
        if slotted:
            return whole.at[who, pl.ds(h * hr, hr), :]
        return whole.at[pl.ds(pl.multiple_of(who * deep + h * hr, hr), hr), :]

    rounds = []
    for w in range(2):
        for dist in range(1, half):
            rounds += [(w, dist, 0), (w, dist, 1)]
        rounds.append((w, half, 0))
    per = fs - 1

    def half_of(way, turn):
        return turn if way == 0 else 1 - turn

    def send(k):
        w, dist, turn = rounds[k]
        for way in range(2):
            h = half_of(way, turn)
            who = owner(way, dist - 1)
            src = slot(w, who, h)
            if dist == 1 and w == 1:
                hr = wo_ref.shape[0] // 2
                src = wo_ref.at[pl.ds(h * hr, hr), :]
            go(remote(src, slot(w, who, h), ring_send.at[way, k], ring_recv.at[way, k],
                      (target[way], me_t)))

    def arrive(k):
        w, dist, turn = rounds[k]
        for way in range(2):
            here = slot(w, owner(way, dist), half_of(way, turn))
            landed(here, ring_send.at[way, k], ring_recv.at[way, k]).wait_recv()
        if dist + 1 < half or (dist + 1 == half and turn == 0):
            send(k + 2)

    up_cols = wu.shape[1]
    deep = wu_ref.shape[0]
    down_rows = wd.shape[1]

    def piece(g, who):
        return wu.at[span(who * deep, deep), :] if g == 0 else wd.at[who]

    def share(g, y):
        if g == 0:
            return wu_ref.at[:, span(y * up_cols, up_cols)]
        return wd_ref.at[span(y * down_rows, down_rows), :]

    def swap_start(g):
        go(remote(share(g, 1 - pair), piece(g, me_f), swap_send.at[g], swap_recv.at[g],
                  (other_f, me_t)))

    def swap_wait(g):
        landed(piece(g, other_f), swap_send.at[g], swap_recv.at[g]).wait_recv()

    line_rounds = [(g, dist, turn) for g in range(2) for dist in range(1, lines) for turn in range(2)]
    per_line = 2 * (lines - 1)

    def line_owner(way, dist, turn):
        at = line - dist if way == 0 else line + dist
        return 2 * at + (pair if turn == 0 else 1 - pair)

    def line_send_round(m, ways=(0, 1)):
        g, dist, turn = line_rounds[m]
        for way in ways:
            who = line_owner(way, dist - 1, turn)
            src = share(g, pair) if dist == 1 and turn == 0 else piece(g, who)
            on = line_next(way) if dist == 1 else jnp.logical_and(line_next(way), line_has(way, dist - 1))
            go(remote(src, piece(g, who), line_send.at[way, m], line_recv.at[way, m],
                      (step_to(way), me_t)), on)

    def line_arrive(m):
        g, dist, turn = line_rounds[m]
        for way in range(2):
            copy = landed(piece(g, line_owner(way, dist, turn)), line_send.at[way, m],
                          line_recv.at[way, m])

            @pl.when(line_has(way, dist))
            def _():
                copy.wait_recv()
            if dist + 1 < lines:
                line_send_round(m + 2, (way,))

    for copy in loads:
        copy.wait()
    send(0)
    send(1)
    own = [None]
    for n, (src, dst) in enumerate((
            (wo_ref, wo.at[me_f]),
            (share(0, pair), piece(0, me_f)),
            (share(1, pair), piece(1, me_f)))):
        copy = pltpu.make_async_copy(src, dst, own_sem.at[n])
        own.append(copy)

    my_rows = span(me_t * rows, rows)

    def norm(source, gain_ref):
        wide = source.astype(F32)
        mean = jnp.mean(wide * wide, axis=-1, keepdims=True)
        return (wide * lax.rsqrt(mean + EPS) * gain_ref[...]).astype(BF16)

    step = 64

    def norm_into(buf, first, source_ref, gain_ref):
        @pl.loop(0, rows // step)
        def _(i):
            at = pl.multiple_of(i * step, step)
            buf[pl.ds(pl.multiple_of(first + at, step), step), :] = norm(
                source_ref[pl.ds(at, step), :], gain_ref)

    def ag_block(t):
        return xn.at[span(t * rows, rows), :]

    ag_copies = [remote(ag_block(me_t), ag_block(me_t), ag_send.at[d - 1], ag_recv.at[d - 1],
                        (me_f, peer(d))) for d in range(1, tp)]

    def ag_start():
        for copy in ag_copies:
            copy.start()

    def ag_wait():
        for d in range(1, tp):
            landed(ag_block(peer(tp - d)), ag_send.at[d - 1], ag_recv.at[d - 1]).wait_recv()

    def project():
        width = proj.shape[1]
        t = tile_of(width)

        @pl.loop(0, width // t)
        def _(j):
            cols = pl.ds(pl.multiple_of(j * t, t), t)
            proj[:, cols] = jnp.dot(xn[...], wq[:, cols], preferred_element_type=F32).astype(BF16)

    def retain():
        kq = heads * DK
        vq = heads * DV
        count = tokens // LENGTH
        for head in range(heads):
            rate = rate_ref[head]

            @pl.loop(0, count)
            def _(n):
                base = pl.multiple_of(n * LENGTH, LENGTH)
                rs = pl.ds(base, LENGTH)
                q = proj[rs, head * DK:(head + 1) * DK]
                k = proj[rs, kq + head * DK:kq + (head + 1) * DK]
                v = proj[rs, 2 * kq + head * DV:2 * kq + (head + 1) * DV]
                g = proj[rs, 2 * kq + vq + head * DV:2 * kq + vq + (head + 1) * DV].astype(F32)
                scores = lax.dot_general(q, k, (((1,), (1,)), ((), ())), preferred_element_type=F32)
                t_at = lax.broadcasted_iota(jnp.int32, (LENGTH, LENGTH), 0)
                s_at = lax.broadcasted_iota(jnp.int32, (LENGTH, LENGTH), 1)
                gap = t_at - s_at
                decay = jnp.exp(-rate * jnp.maximum(gap, 0).astype(F32)) * (DK ** -0.5)
                scores = jnp.where(gap >= 0, scores * decay, 0.0).astype(BF16)
                mixed = jnp.dot(scores, v, preferred_element_type=F32)
                mean = jnp.mean(mixed, axis=-1, keepdims=True)
                off = mixed - mean
                var = jnp.mean(off * off, axis=-1, keepdims=True)
                grouped = off * lax.rsqrt(var + EPS)
                gated[rs, head * DV:(head + 1) * DV] = (g / (1.0 + jnp.exp(-g)) * grouped).astype(BF16)

    def mix_block(x, c):
        return part1.at[span((2 * x + c) * rows, rows), :]

    def mix_out():
        cols = wo.shape[2]

        @pl.loop(0, fs)
        def _(j):
            part1[:, span(j * cols, cols)] = jnp.dot(
                gated[...], wo[j], preferred_element_type=F32).astype(BF16)
        order = [e % chips for e in range(1, chips + 1)]
        for e in order:
            x = (chip + e) % chips
            go(remote(mix_block(x, 1 - core), core1.at[e], core1_send.at[e], core1_recv.at[e],
                      (me_f, other_t)))
        for e in order:
            landed(core1.at[e], core1_send.at[e], core1_recv.at[e]).wait_recv()
            if e:
                first = beside(e) * rows

                @pl.loop(0, rows // step)
                def _(i):
                    at = pl.ds(pl.multiple_of(first + i * step, step), step)
                    more = core1[e, span(i * step, step), :].astype(F32)
                    part1[at, :] = (part1[at, :].astype(F32) + more).astype(BF16)
                go(remote(ag_mix(beside(e)), chip1.at[e - 1], chip1_send.at[e - 1],
                          chip1_recv.at[e - 1], (me_f, beside(e))))

    def ag_mix(t):
        return part1.at[span(t * rows, rows), :]

    def mix_end():
        for e in range(1, chips):
            landed(chip1.at[e - 1], chip1_send.at[e - 1], chip1_recv.at[e - 1]).wait_recv()

        @pl.loop(0, rows // step)
        def _(i):
            at = span(i * step, step)
            total = part1[pl.ds(pl.multiple_of(me_t * rows + i * step, step), step), :].astype(F32)
            total = total + core1[0, at, :].astype(F32)
            for e in range(1, chips):
                total = total + chip1[e - 1, at, :].astype(F32)
            sum_ = (resid_ref[at, :].astype(F32) + total).astype(BF16)
            after[at, :] = sum_
            xn2[pl.ds(pl.multiple_of(block(pair, me_t) * rows + i * step, step), step), :] = norm(
                sum_, mlp_gain_ref)

    def block(y, t):
        return (t % 2) * (2 * chips) + y * chips + t // 2

    def wide(y, t, part=None):
        first = block(y, t) * rows
        hr = rows // 2
        if part is None:
            return xn2.at[span(first, rows), :]
        return xn2.at[pl.ds(pl.multiple_of(first + part * hr, hr), hr), :]

    more_chips = chips - 1
    pieces = 1 + 3 * more_chips

    def all_copy(n, ref, where):
        go(remote(ref, ref, all_send.at[n], all_recv.at[n], where))

    def all_landed(n, ref):
        landed(ref, all_send.at[n], all_recv.at[n]).wait_recv()

    def across(n, ref):
        all_copy(pieces + n, ref, (me_f, other_t))

    def all_first():
        ref = wide(pair, me_t)
        all_copy(0, ref, (other_f, me_t))
        for e in range(1, chips):
            all_copy(e, ref, (me_f, beside(e)))
        all_copy(2 * pieces, ref, (me_f, other_t))

    def all_second():
        ref = wide(1 - pair, me_t)
        all_landed(0, ref)
        for e in range(1, chips):
            all_copy(more_chips + e, wide(1 - pair, me_t, 0), (me_f, beside(e)))
        across(0, ref)
        for e in range(1, chips):
            t = beside(chips - e)
            all_landed(e, wide(pair, t))
            all_copy(2 * more_chips + e, wide(pair, t, 1), (other_f, me_t))
            across(e, wide(pair, t))

    def all_third():
        for part in range(2):
            for e in range(1, chips):
                n = (1 + part) * more_chips + e
                ref = wide(1 - pair, beside(chips - e), part)
                all_landed(n, ref)
                across(n, ref)
        all_landed(2 * pieces, wide(pair, other_t))
        all_landed(pieces, wide(1 - pair, other_t))
        for e in range(1, chips):
            t = 2 * ((chip + chips - e) % chips) + 1 - core
            all_landed(pieces + e, wide(pair, t))
            for part in range(2):
                all_landed(pieces + (1 + part) * more_chips + e, wide(1 - pair, t, part))

    def lift():
        t = tile_of(up_cols)

        @pl.loop(0, 2)
        def _(i):
            at = span(i * tokens, tokens)

            @pl.loop(0, up_cols // t)
            def _(j):
                cols = span(j * t, t)
                up = jnp.maximum(jnp.dot(xn2[at, :], wu[:, cols], preferred_element_type=F32), 0.0)
                hidden[at, cols] = (up * up).astype(BF16)

    cw = wd.shape[2]
    r2 = 2 * chips - 1

    def mlp_copies(who):
        cols = span(who * cw, cw)
        first = core * tokens
        side = remote(part2.at[span((1 - core) * tokens, tokens), cols], xn.at[:, cols],
                      core2_send.at[who], core2_recv.at[who], (me_f, other_t))
        side_in = landed(xn.at[:, cols], core2_send.at[who], core2_recv.at[who])
        outs, ins = [], []
        n = 0
        for dy in range(2):
            for e in range(chips):
                if dy == 0 and e == 0:
                    continue
                y = pair if dy == 0 else 1 - pair
                t = beside(e)
                dst = chip2.at[n, :, cols]
                outs.append(remote(part2.at[span(block(y, t) * rows, rows), cols], dst,
                                   chip2_send.at[n, who], chip2_recv.at[n, who],
                                   (me_f if dy == 0 else other_f, t)))
                ins.append(landed(dst, chip2_send.at[n, who], chip2_recv.at[n, who]))
                n += 1
        return side, side_in, outs, ins

    finals = []

    def lower(who, on=None):
        side, side_in, outs, ins = mlp_copies(who)
        cols = span(who * cw, cw)
        mine = block(pair, me_t) * rows

        def run():
            @pl.loop(0, 2)
            def _(i):
                at = span(((1 - core) * (1 - i) + core * i) * tokens, tokens)
                part2[at, cols] = jnp.dot(
                    hidden[at, :], wd[who], preferred_element_type=F32).astype(BF16)

                @pl.when(i == 0)
                def _():
                    side.start()
            side_in.wait_recv()

            @pl.loop(0, tokens // 128)
            def _(i):
                at = pl.ds(pl.multiple_of(core * tokens + i * 128, 128), 128)
                more = xn[span(i * 128, 128), cols].astype(F32)
                part2[at, cols] = (part2[at, cols].astype(F32) + more).astype(BF16)
            for copy in outs:
                copy.start()

        def end():
            for copy in ins:
                copy.wait_recv()
            total = part2[span(mine, rows), cols].astype(F32)
            for n in range(r2):
                total = total + chip2[n, :, cols].astype(F32)
            out_ref[:, cols] = (after[:, cols].astype(F32) + total).astype(BF16)
            side.wait_send()
            for copy in outs:
                copy.wait_send()

        if on is None:
            run()
        else:
            pl.when(on)(run)
        finals.append((end, on))

    norm_into(xn, me_t * rows, resid_ref, mix_gain_ref)
    ag_start()
    for copy in own[1:]:
        copy.start()

    own_at = {per - 3: [per], per - 2: [per + 1]}

    for k in range(2 * per):
        arrive(k)
        for extra in own_at.get(k, ()):
            send(extra)
        if k == per - 1:
            line_send_round(0)
            swap_start(0)
            ag_wait()
            project()
        elif k == per + 1:
            retain()
        elif k == 2 * per - 4:
            swap_wait(0)
            line_send_round(1)
            swap_start(1)
        elif k == 2 * per - 1:
            own[1].wait()
            mix_out()

    last_d = per_line - 2
    for m in range(2 * per_line):
        line_arrive(m)
        if m == last_d - 1:
            line_send_round(per_line)
        elif m == last_d:
            swap_wait(1)
            line_send_round(per_line + 1)
        if m == per_line + (-3):
            for copy in ag_copies:
                copy.wait_send()
            mix_end()
            all_first()
        elif m == per_line + (-1):
            all_second()
        elif m == per_line:
            own[2].wait()
            own[3].wait()
            all_third()
            lift()
            lower(me_f)
            lower(other_f)
        if m >= per_line:
            _, dist, turn = line_rounds[m]
            for way in range(2):
                lower(line_owner(way, dist, turn), line_has(way, dist))

    for end, on in finals:
        if on is None:
            end()
        else:
            pl.when(on)(end)
    for copy, on in started:
        if on is None:
            copy.wait_send()
        else:
            pl.when(on)(copy.wait_send)


def on_device(fs, tp, resid, mix_gain, w_query, w_key, w_value, w_gate, w_output, decay_rate,
              mlp_gain, w_up, w_down):
    rows, width = resid.shape
    tokens = rows * tp
    in_width = w_query.shape[1] + w_key.shape[1] + w_value.shape[1] + w_gate.shape[1]
    chips = tp // 2
    wide = 2 * (1 + 3 * (chips - 1)) + 1
    vmem = pl.BlockSpec(memory_space=pltpu.VMEM)
    hbm = pl.BlockSpec(memory_space=pl.ANY)
    dma = pltpu.SemaphoreType.DMA
    cols = width // fs
    return pl.pallas_call(
        functools.partial(kernel, fs, tp),
        out_shape=jax.ShapeDtypeStruct((rows, width), BF16),
        in_specs=[vmem] * 3 + [pl.BlockSpec(memory_space=pltpu.SMEM)] + [hbm] * 7,
        out_specs=vmem,
        scratch_shapes=[
            pltpu.VMEM((width, in_width), BF16),
            pltpu.VMEM((fs, w_output.shape[0], cols), BF16),
            pltpu.VMEM((width, w_up.shape[1] // 2), BF16),
            pltpu.VMEM((fs, w_down.shape[0] // 2, cols), BF16),
            pltpu.VMEM((tokens, width), BF16),
            pltpu.VMEM((2 * tokens, width), BF16),
            pltpu.VMEM((tokens, in_width), BF16),
            pltpu.VMEM((tokens, w_output.shape[0]), BF16),
            pltpu.VMEM((2 * tokens, w_up.shape[1] // 2), BF16),
            pltpu.VMEM((tokens, width), BF16),
            pltpu.VMEM((chips, rows, width), BF16),
            pltpu.VMEM((chips - 1, rows, width), BF16),
            pltpu.VMEM((2 * tokens, width), BF16),
            pltpu.VMEM((2 * chips - 1, rows, width), BF16),
            pltpu.VMEM((rows, width), BF16),
            dma((2, 2 * (fs - 1))),
            dma((2, 2 * (fs - 1))),
            dma((3,)),
            dma((4,)),
            dma((tp - 1,)),
            dma((tp - 1,)),
            dma((2, 2 * (fs - 2))),
            dma((2, 2 * (fs - 2))),
            dma((2,)),
            dma((2,)),
            dma((chips,)),
            dma((chips,)),
            dma((chips - 1,)),
            dma((chips - 1,)),
            dma((wide,)),
            dma((wide,)),
            dma((fs,)),
            dma((fs,)),
            dma((2 * chips - 1, fs)),
            dma((2 * chips - 1, fs)),
        ],
        compiler_params=pltpu.CompilerParams(
            collective_id=0, has_side_effects=True, vmem_limit_bytes=67043328),
    )(resid, mix_gain[None, :], mlp_gain[None, :], decay_rate, w_query, w_key, w_value,
      w_gate, w_output, w_up, w_down)


def solution(mesh):
    placed = (
        P(("fs", "tp"), None),
        P(),
        P("fs", "tp"),
        P("fs", "tp"),
        P("fs", "tp"),
        P("fs", "tp"),
        P("tp", "fs"),
        P("tp"),
        P(),
        P("fs", "tp"),
        P("tp", "fs"),
    )
    sizes = dict(mesh.shape)
    return jax.shard_map(
        functools.partial(on_device, sizes["fs"], sizes["tp"]), mesh=mesh, in_specs=placed,
        out_specs=P(("fs", "tp"), None), check_vma=False)
```
